32 devices in a mesh: ep: 8 (over z, x), tp: 4 (over y, core).
Axes of the slice: x: 2, y: 2, z: 4, core: 2. Of those that a mesh axis runs over, the one named last changes fastest.
Arguments:
- tokens: bfloat16 [4096, 4096], P('ep', 'tp'), may hold values from -6 to 6
- cotangent: bfloat16 [4096, 4096], P('ep', 'tp'), may hold values from -6 to 6
- expert_ids: int32 [4096, 2], P('ep'), may hold values from 0 to 15, as said below
- route_weight: float32 [4096, 2], P('ep'), may hold values from 0.1 to 1
- gate_weight: bfloat16 [16, 4096, 512], P('ep', 'tp'), may hold values from -0.09375 to 0.09375
- up_weight: bfloat16 [16, 4096, 512], P('ep', 'tp'), may hold values from -0.09375 to 0.09375
- down_weight: bfloat16 [16, 512, 4096], P('ep', None, 'tp'), may hold values from -0.25 to 0.25
- saved_gate: bfloat16 [8, 16, 128, 512], P(None, 'ep'), may hold values from -6 to 6
- saved_up: bfloat16 [8, 16, 128, 512], P(None, 'ep'), may hold values from -6 to 6
Outputs:
- token_grad: bfloat16 [4096, 4096], P('ep', 'tp')
- route_grad: float32 [4096, 2], P('ep')
- gate_weight_grad: bfloat16 [16, 4096, 512], P('ep', 'tp')
- up_weight_grad: bfloat16 [16, 4096, 512], P('ep', 'tp')
- down_weight_grad: bfloat16 [16, 512, 4096], P('ep', None, 'tp')
The draws below stay inside these ranges and needn't reach their ends.
Inputs may be any that keep to these rules, and one draw needn't show every extreme that they name: `expert_ids`: each row names 2 different experts of one group of 4 consecutive experts. In each aligned block of 512 rows (the rows of one index of ep) no expert is named more than 128 times; the experts of one group, drawn from the seed, are named exactly 128 times in every block, and other experts may reach 128 too.
All inputs are finite; a program needn't handle non-finite values.
Results may differ from the reference program's by a relative error of at most 0.02.
Values may be sent and summed in bfloat16 or wider, within the bound.
A program may use at most 128 MiB of HBM per device.

```python
import jax
import jax.numpy as jnp
from jax import lax

D = 4096
F = 512
TOP_K = 2
E_GROUP = 4
TOK_DEV = 512
BLOCKS = 8
EXPERTS = 16
GROUPS = 4
CAP = 128
TOKENS = 4096
N_TP = 4


def block_choices(block_key, hot_group):
    first_key, second_key, third_key, fourth_key, fifth_key = jax.random.split(block_key, 5)
    offsets = jax.random.randint(first_key, (GROUPS,), 0, E_GROUP)
    second_group = (hot_group + 1 + jax.random.randint(second_key, (), 0, GROUPS - 1)) % GROUPS
    group_range = jnp.arange(GROUPS, dtype=jnp.int32)
    taken = ((group_range == hot_group) | (group_range == second_group)).astype(jnp.int32)
    order_keys = jax.random.permutation(third_key, GROUPS).astype(jnp.int32) + GROUPS * taken
    ranked = jnp.argsort(order_keys).astype(jnp.int32)
    rest_groups = ranked[:GROUPS - 2]
    busiest = CAP * E_GROUP // 2
    places = jnp.arange(TOK_DEV, dtype=jnp.int32)
    remain = jnp.maximum(places - 2 * busiest, 0)
    spread_group = rest_groups[remain % (GROUPS - 2)]
    group = jnp.where(places < busiest, hot_group, jnp.where(places < 2 * busiest, second_group, spread_group))
    inner = jnp.where(places < 2 * busiest, places % busiest, remain // (GROUPS - 2))
    first = group * E_GROUP + (inner + offsets[group]) % E_GROUP
    second = group * E_GROUP + (inner + 1 + offsets[group]) % E_GROUP
    flips = jax.random.randint(fourth_key, (TOK_DEV,), 0, 2)
    paired = jnp.stack([jnp.where(flips == 1, second, first), jnp.where(flips == 1, first, second)], axis=1)
    shuffle = jax.random.permutation(fifth_key, TOK_DEV)
    return paired[shuffle]


def draw_expert_ids(key, part):
    hot_group = jax.random.randint(jax.random.fold_in(key, 11), (), 0, GROUPS)
    block_keys = jax.random.split(jax.random.fold_in(key, 12), TOKENS // TOK_DEV)
    chosen = jax.vmap(lambda block_key: block_choices(block_key, hot_group))(block_keys)
    return chosen.reshape(TOKENS, TOP_K).astype(jnp.int32)


def shard_levels(stream_key, dims, pieces, least, top_value):
    loudness = 1.0
    for dim, parts in pieces:
        heights = jax.random.uniform(jax.random.fold_in(jax.random.fold_in(stream_key, 6), dim), (parts,), jnp.float32, least / len(pieces), top_value / len(pieces))
        loudness = loudness * jnp.repeat(jnp.exp(heights), dims[dim] // parts).reshape((-1,) + (1,) * (len(dims) - 1 - dim))
    return loudness


def scatter_about(key, dims, spread, reach, shards=(), held_as=jnp.bfloat16):
    gain = shard_levels(key, dims, shards, -0.22, 0.18) if shards else 1.0
    values = jax.random.normal(key, dims, jnp.float32) * spread * gain
    return jnp.minimum(jnp.maximum(values, -reach), reach).astype(held_as)


def setup_inputs(seed: int = 0) -> dict:
    seeds = jax.random.split(jax.random.key(seed), 10)
    return {
        "tokens": scatter_about(seeds[0], (TOKENS, D), 1.0, 6.0, ((0, 8), (1, 4))),
        "cotangent": scatter_about(seeds[1], (TOKENS, D), 1.0, 6.0, ((0, 8), (1, 4))),
        "expert_ids": draw_expert_ids(jax.random.fold_in(seeds[9], 71), 0),
        "route_weight": jnp.clip(0.1 + 0.9 * jax.random.uniform(seeds[3], (TOKENS, TOP_K), jnp.float32) ** shard_levels(seeds[3], (TOKENS, TOP_K), ((0, 8),), -0.2, 0.2), 0.1, 1.0),
        "gate_weight": scatter_about(seeds[4], (EXPERTS, D, F), D ** -0.5, 0.09375, ((0, 8), (1, 4))),
        "up_weight": scatter_about(seeds[5], (EXPERTS, D, F), D ** -0.5, 0.09375, ((0, 8), (1, 4))),
        "down_weight": scatter_about(seeds[6], (EXPERTS, F, D), F ** -0.5, 0.25, ((0, 8), (2, 4))),
        "saved_gate": scatter_about(seeds[7], (BLOCKS, EXPERTS, CAP, F), 1.5, 6.0, ((1, 8),)),
        "saved_up": scatter_about(seeds[8], (BLOCKS, EXPERTS, CAP, F), 1.0, 6.0, ((1, 8),)),
    }


def slot_layout(expert_ids):
    assigned = TOK_DEV * TOP_K
    flat_ids = expert_ids.reshape(BLOCKS, assigned)
    onehot = (flat_ids[:, :, None] == jnp.arange(EXPERTS, dtype=jnp.int32)[None, None, :]).astype(jnp.int32)
    earlier = jnp.cumsum(onehot, axis=1) - onehot
    slot_index = jnp.sum(earlier * onehot, axis=2).astype(jnp.int32)
    position = (flat_ids * CAP + slot_index).astype(jnp.int32)
    block_index = jnp.broadcast_to(jnp.arange(BLOCKS, dtype=jnp.int32)[:, None], (BLOCKS, assigned))
    numbers = jnp.broadcast_to(jnp.arange(assigned, dtype=jnp.int32)[None, :], (BLOCKS, assigned))
    slot_table = jnp.full((BLOCKS, EXPERTS * CAP), assigned, jnp.int32).at[block_index, position].set(numbers)
    return position, slot_table


def reference(tokens, cotangent, expert_ids, route_weight, gate_weight, up_weight, down_weight, saved_gate, saved_up):
    assigned = TOK_DEV * TOP_K
    model_width = tokens.shape[1]
    hidden_units = gate_weight.shape[2]
    width_local = model_width // N_TP
    position, slot_table = slot_layout(expert_ids)
    filled = slot_table < assigned
    picked = jnp.minimum(slot_table, assigned - 1)
    block_base = jnp.arange(BLOCKS, dtype=jnp.int32)[:, None]
    token_row = jnp.where(filled, block_base * TOK_DEV + picked // TOP_K, TOKENS).astype(jnp.int32)
    slot_weight = jnp.where(filled, route_weight.reshape(-1)[block_base * assigned + picked], jnp.float32(0.0))
    token_row = jnp.transpose(token_row.reshape(BLOCKS, EXPERTS, CAP), (1, 0, 2))
    slot_weight = jnp.transpose(slot_weight.reshape(BLOCKS, EXPERTS, CAP), (1, 0, 2))
    padded_tokens = jnp.concatenate([tokens, jnp.zeros((1, model_width), tokens.dtype)], axis=0)
    padded_cot = jnp.concatenate([cotangent, jnp.zeros((1, model_width), cotangent.dtype)], axis=0)
    gate_saved = jnp.transpose(saved_gate, (1, 0, 2, 3))
    up_saved = jnp.transpose(saved_up, (1, 0, 2, 3))

    def expert_step(totals, inputs):
        gate_one, up_one, down_one, pre_gate, pre_up, row_index, weight_slot = inputs
        rows_flat = row_index.reshape(-1)
        inputs_rows = padded_tokens[rows_flat]
        grads_in = padded_cot[rows_flat]
        gate_pre = pre_gate.astype(jnp.float32).reshape(-1, hidden_units)
        up_pre = pre_up.astype(jnp.float32).reshape(-1, hidden_units)
        sigmoid_gate = jax.nn.sigmoid(gate_pre)
        hidden = gate_pre * sigmoid_gate * up_pre
        hidden_bf = hidden.astype(jnp.bfloat16)
        partial_terms = jnp.einsum("rnd,fnd->rnf",
                                   grads_in.reshape(-1, N_TP, width_local).astype(jnp.float32),
                                   down_one.reshape(hidden_units, N_TP, width_local).astype(jnp.float32))
        rounded = lax.optimization_barrier(partial_terms.astype(jnp.bfloat16))
        back_grad = jnp.sum(rounded.astype(jnp.float32), axis=1)
        expert_out = jnp.dot(hidden_bf, down_one, preferred_element_type=jnp.float32)
        scores = jnp.sum(expert_out * grads_in.astype(jnp.float32), axis=1)
        weights = weight_slot.reshape(-1)[:, None]
        grad_hidden = weights * back_grad
        grad_up_pre = (grad_hidden * gate_pre * sigmoid_gate).astype(jnp.bfloat16)
        grad_gate_pre = (grad_hidden * up_pre * sigmoid_gate * (1.0 + gate_pre * (1.0 - sigmoid_gate))).astype(jnp.bfloat16)
        weighted = (weights * hidden).astype(jnp.bfloat16)
        gate_grad_one = jnp.dot(inputs_rows.T, grad_gate_pre, preferred_element_type=jnp.float32).astype(jnp.bfloat16)
        up_grad_one = jnp.dot(inputs_rows.T, grad_up_pre, preferred_element_type=jnp.float32).astype(jnp.bfloat16)
        down_grad_one = jnp.dot(weighted.T, grads_in, preferred_element_type=jnp.float32).astype(jnp.bfloat16)
        slot_grad = (jnp.dot(grad_gate_pre, gate_one.T, preferred_element_type=jnp.float32)
                     + jnp.dot(grad_up_pre, up_one.T, preferred_element_type=jnp.float32)).astype(jnp.bfloat16)
        totals = totals.at[rows_flat].add(slot_grad.astype(jnp.float32))
        return totals, (gate_grad_one, up_grad_one, down_grad_one, scores)

    initial = jnp.zeros((TOKENS + 1, model_width), jnp.float32)
    totals, outputs = lax.scan(expert_step, initial,
                               (gate_weight, up_weight, down_weight, gate_saved, up_saved, token_row, slot_weight))
    gate_weight_grad, up_weight_grad, down_weight_grad, scores = outputs
    token_grad = totals[:TOKENS].astype(jnp.bfloat16)
    score_table = jnp.transpose(scores.reshape(EXPERTS, BLOCKS, CAP), (1, 0, 2)).reshape(BLOCKS, EXPERTS * CAP)
    route_grad = jnp.take_along_axis(score_table, position, axis=1).reshape(TOKENS, TOP_K)
    return token_grad, route_grad, gate_weight_grad, up_weight_grad, down_weight_grad
```

```python
import jax
import jax.numpy as jnp
from jax import lax
from jax.sharding import PartitionSpec as P

E_GROUP = 4
BACK_CHUNKS = 2
OUT_CHUNKS = 2
BF = jnp.bfloat16
F32 = jnp.float32


def dot32(spec, a, b):
    return jnp.einsum(spec, a, b, preferred_element_type=F32)


def sum_over_tp(part):
    if lax.axis_size("tp") != 4 or part.shape[0] % 2:
        return lax.psum(part, "tp").astype(F32)
    first = lax.axis_index("tp") % 2 == 0
    cores = [(i, i ^ 1) for i in range(4)]
    chips = [(i, i ^ 2) for i in range(4)]
    half = part.shape[0] // 2
    low, high = part[:half], part[half:]
    got = lax.ppermute(jnp.where(first, high, low), "tp", cores)
    mine = (jnp.where(first, low, high).astype(F32) + got.astype(F32)).astype(BF)
    other = lax.ppermute(mine, "tp", chips)
    mine = mine.astype(F32) + other.astype(F32)
    theirs = lax.ppermute(mine, "tp", cores)
    return jnp.concatenate(
        [jnp.where(first, mine, theirs), jnp.where(first, theirs, mine)], axis=0
    )


def local(
    tokens,
    cotangent,
    expert_ids,
    route_weight,
    gate_weight,
    up_weight,
    down_weight,
    saved_gate,
    saved_up,
):
    sources = lax.axis_size("ep")
    tok_rows, width = tokens.shape
    top_k = expert_ids.shape[1]
    local_experts = gate_weight.shape[0]
    all_experts = local_experts * sources
    capacity = saved_gate.shape[2]
    hidden_units = gate_weight.shape[2]
    span = E_GROUP // local_experts
    groups = sources // span
    group_cap = min(E_GROUP * capacity // top_k, tok_rows)
    slots = local_experts * capacity
    lane = lax.axis_index("ep") % span
    columns = [[g * span + p for g in range(groups)] for p in range(span)]

    def across(x):
        return lax.all_to_all(
            x, "ep", split_axis=0, concat_axis=0, tiled=True, axis_index_groups=columns
        )

    def shift(x, by):
        pairs = [
            (g * span + p, g * span + (p + by) % span) for g in range(groups) for p in range(span)
        ]
        return lax.ppermute(x, "ep", pairs)

    def of_lane(x, j):
        split = x.reshape((groups, span) + x.shape[1:])
        return lax.dynamic_index_in_dim(split, (lane + j) % span, axis=1, keepdims=False)

    hits = expert_ids[:, :, None] == jnp.arange(all_experts, dtype=jnp.int32)
    named = jnp.any(hits, axis=1)
    token_weight = jnp.sum(jnp.where(hits, route_weight[:, :, None], 0.0), axis=1)
    group = expert_ids[:, 0] // E_GROUP
    in_group = group[:, None] == jnp.arange(groups, dtype=jnp.int32)
    marks = jnp.concatenate([named, in_group], axis=1).astype(BF)
    ticks = jnp.arange(tok_rows, dtype=jnp.int32)
    earlier = (ticks[None, :] < ticks[:, None]).astype(BF)
    counts = dot32("ts,sm->tm", earlier, marks)
    rank = jnp.sum(jnp.where(in_group, counts[:, all_experts:], 0.0), axis=1)
    slot_key = jnp.where(named, counts[:, :all_experts], -1.0)
    place = group * group_cap + rank.astype(jnp.int32)
    pick = (
        jnp.arange(groups * group_cap, dtype=jnp.int32)[:, None] == place[None, :]
    ).astype(BF)

    def pack(x):
        return dot32("rt,td->rd", pick, x).astype(BF).reshape(groups, group_cap, x.shape[1])

    slot_hit = slot_key[:, :, None] == jnp.arange(capacity, dtype=F32)
    rank_table = jnp.sum(jnp.where(slot_hit, rank[:, None, None] + 1.0, 0.0), axis=0)
    weight_table = jnp.sum(jnp.where(slot_hit, token_weight[:, :, None], 0.0), axis=0)
    tables = jnp.stack(
        [
            rank_table.reshape(sources, slots),
            weight_table.reshape(sources, slots),
        ],
        axis=1,
    )

    step = width // BACK_CHUNKS
    cot_parts = [[] for _ in range(span)]
    token_parts = [[] for _ in range(span)]
    before = None
    for source, parts in ((cotangent, cot_parts), (tokens, token_parts)):
        for k in range(BACK_CHUNKS):
            piece = pack(source[:, k * step : (k + 1) * step])
            if before is None:
                pass
            elif len(cot_parts[0]) == 1:
                tables, before = lax.optimization_barrier((tables, before))
                tables = lax.all_to_all(tables, "ep", split_axis=0, concat_axis=0, tiled=True)
                piece, tables, before = lax.optimization_barrier((piece, tables, before))
                for (held, at), value in zip(spots, before):
                    held[at] = value
            else:
                piece, before = lax.optimization_barrier((piece, before))
                for (held, at), value in zip(spots, before):
                    held[at] = value
            parts[0].append(across(piece))
            passed_on = [(parts[j], k) for j in range(1, span)]
            for j in range(1, span):
                if source is cotangent or k + 1 < BACK_CHUNKS:
                    parts[j].append(shift(parts[0][k], -j))
            spots = [(parts[0], k)] + (last_on if before is not None else [])
            before = [held[at] for held, at in spots]
            last_on = passed_on

    both_weight = jnp.concatenate([gate_weight, up_weight], axis=2)

    spread, weights, cot_slots, partial = [], [], [], []
    for j in range(span):
        table = of_lane(tables, j)
        spread.append(
            (table[:, 0, :, None] - 1.0 == jnp.arange(group_cap, dtype=F32)).astype(BF)
        )
        weights.append(table[:, 1].reshape(groups, local_experts, capacity, 1))
        cot_rows = jnp.concatenate(cot_parts[j], axis=2)
        rows = dot32("gst,gtd->gsd", spread[j], cot_rows).astype(BF)
        cot_slots.append(rows.reshape(groups, local_experts, capacity, width))
        partial.append(dot32("gecd,efd->gecf", cot_slots[j], down_weight).astype(BF))

    summed = [sum_over_tp(part) for part in partial]

    both_grad, weighted, scores = [], [], []
    for j in range(span):
        gate_pre = of_lane(saved_gate, j).astype(F32)
        up_pre = of_lane(saved_up, j).astype(F32)
        back = summed[j]
        sigmoid_gate = jax.nn.sigmoid(gate_pre)
        hidden = gate_pre * sigmoid_gate * up_pre
        scores.append(jnp.sum(hidden.astype(BF).astype(F32) * back, axis=3))
        grad_hidden = weights[j] * back
        grad_up = (grad_hidden * gate_pre * sigmoid_gate).astype(BF)
        grad_gate = (
            grad_hidden * up_pre * sigmoid_gate * (1.0 + gate_pre * (1.0 - sigmoid_gate))
        ).astype(BF)
        both_grad.append(jnp.concatenate([grad_gate, grad_up], axis=3))
        weighted.append((weights[j] * hidden).astype(BF))

    both_grad, token_parts = lax.optimization_barrier((both_grad, token_parts))

    score_lanes = jnp.stack(scores, axis=1)
    score_send = jnp.stack(
        [
            lax.dynamic_index_in_dim(score_lanes, (q - lane) % span, axis=1, keepdims=False)
            for q in range(span)
        ],
        axis=1,
    ).reshape(sources, local_experts, capacity)

    step = width // OUT_CHUNKS

    def rows_of(j, k):
        weight_k = both_weight[:, k * step : (k + 1) * step]
        grad = dot32("gecf,edf->gecd", both_grad[j], weight_k).astype(BF)
        return dot32("gst,gsd->gtd", spread[j], grad.reshape(groups, slots, step))

    sends = [[rows_of(j, k).astype(BF) for j in range(1, span)] for k in range(OUT_CHUNKS)]
    sends[0], score_send = lax.optimization_barrier((sends[0], score_send))
    ahead = lax.all_to_all(score_send, "ep", split_axis=0, concat_axis=0, tiled=True)
    out_parts = []
    for k in range(OUT_CHUNKS):
        others = [shift(x, j + 1) for j, x in enumerate(sends[k])]
        total = rows_of(0, k)
        if k + 1 == OUT_CHUNKS:
            late, others = lax.optimization_barrier((token_parts[0][-1], others))
            token_parts[0][-1] = late
            for j in range(1, span):
                token_parts[j].append(shift(late, -j))
        for other in others:
            total = total + other.astype(F32)
        total = total.astype(BF)
        if k == 0:
            total, score_back = lax.optimization_barrier((total, ahead))
        if k + 1 < OUT_CHUNKS:
            total, sends[k + 1] = lax.optimization_barrier((total, sends[k + 1]))
        out_parts.append(across(total))
    token_grad = jnp.concatenate(
        [
            dot32("rt,rd->td", pick, part.reshape(groups * group_cap, step)).astype(BF)
            for part in out_parts
        ],
        axis=1,
    )

    score_table = score_back.reshape(all_experts, capacity)
    choice_hits = hits.reshape(-1, all_experts)
    choice_slot = jnp.sum(jnp.where(hits, counts[:, None, :all_experts], 0.0), axis=2)
    choice_rows = jnp.dot(
        choice_hits.astype(F32), score_table, precision=lax.Precision.HIGHEST
    )
    choice_slot_hit = choice_slot.reshape(-1, 1) == jnp.arange(capacity, dtype=F32)
    route_grad = jnp.sum(jnp.where(choice_slot_hit, choice_rows, 0.0), axis=1)
    route_grad = route_grad.reshape(tok_rows, top_k)

    all_tokens = jnp.concatenate(
        [
            dot32("gst,gtd->gsd", spread[j], jnp.concatenate(token_parts[j], axis=2))
            .astype(BF)
            .reshape(groups, local_experts, capacity, width)
            for j in range(span)
        ],
        axis=0,
    )
    all_cot = jnp.concatenate(cot_slots, axis=0)
    all_both = jnp.concatenate(both_grad, axis=0)
    all_weighted = jnp.concatenate(weighted, axis=0)
    gate_weight_grad = dot32("secd,secf->edf", all_tokens, all_both[..., :hidden_units]).astype(BF)
    up_weight_grad = dot32("secd,secf->edf", all_tokens, all_both[..., hidden_units:]).astype(BF)
    down_weight_grad = dot32("secf,secd->efd", all_weighted, all_cot).astype(BF)
    return (token_grad, route_grad, gate_weight_grad, up_weight_grad, down_weight_grad)


def solution(mesh):
    in_specs = (
        P("ep", "tp"),
        P("ep", "tp"),
        P("ep", None),
        P("ep", None),
        P("ep", "tp", None),
        P("ep", "tp", None),
        P("ep", None, "tp"),
        P(None, "ep", None, None),
        P(None, "ep", None, None),
    )
    out_specs = (
        P("ep", "tp"),
        P("ep", None),
        P("ep", "tp", None),
        P("ep", "tp", None),
        P("ep", None, "tp"),
    )
    return jax.shard_map(local, mesh=mesh, in_specs=in_specs, out_specs=out_specs, check_vma=False)
```
